32 devices in a mesh: fs: 8 (over z, y), tp: 4 (over x, core).
Axes of the slice: x: 2, y: 2, z: 4, core: 2. Of those that a mesh axis runs over, the one named last changes fastest.
Arguments:
- hidden_in: bfloat16 [512, 4096], P(None, 'tp'), may hold values from -6 to 6
- up_act: bfloat16 [512, 12288], P('tp', 'fs'), may hold values from -6 to 6
- up_val: bfloat16 [512, 12288], P('tp', 'fs'), may hold values from -6 to 6
- cotangent: bfloat16 [512, 4096], P('tp'), may hold values from -6 to 6
- w_act: bfloat16 [4096, 12288], P('tp', 'fs'), may hold values from -0.09375 to 0.09375
- w_val: bfloat16 [4096, 12288], P('tp', 'fs'), may hold values from -0.09375 to 0.09375
- w_down: bfloat16 [12288, 4096], P('fs', 'tp'), may hold values from -0.0546875 to 0.0546875
- conv_act: bfloat16 [3, 12288], P(None, 'fs'), may hold values from -3 to 3
- conv_val: bfloat16 [3, 12288], P(None, 'fs'), may hold values from -3 to 3
- bias_act: bfloat16 [12288], P('fs'), may hold values from -3 to 3
- bias_val: bfloat16 [12288], P('fs'), may hold values from -3 to 3
Outputs:
- grad_input: bfloat16 [512, 4096], P(('tp', 'fs'))
- grad_w_act: float32 [4096, 12288], P('tp', 'fs')
- grad_w_val: float32 [4096, 12288], P('tp', 'fs')
- grad_w_down: float32 [12288, 4096], P('fs', 'tp')
- grad_conv_act: float32 [3, 12288], P(None, 'fs')
- grad_conv_val: float32 [3, 12288], P(None, 'fs')
- grad_bias_act: float32 [12288], P('fs')
- grad_bias_val: float32 [12288], P('fs')
- rows_act: float32 [4096], P('tp')
- rows_val: float32 [4096], P('tp')
- rows_down: float32 [12288], P('fs')
- conv_rows: float32 [2, 3], replicated
The draws below stay inside these ranges and needn't reach their ends.
All inputs are finite; a program needn't handle non-finite values.
Results may differ from the reference program's by a relative error of at most 0.0057.
Values may be sent and summed in bfloat16 or wider, within the bound.
A program may use at most 128 MiB of HBM per device.

```python
import jax
import jax.numpy as jnp
from jax import lax

D = 4096
FF = 12288
KW = 3
TOKENS = 512


def with_spikes(result, own_key, source, target, parts, factor):
    owner, partner = [(jnp.arange(result.shape[axis_at]) // (result.shape[axis_at] // parts)).reshape([-1 if axis == axis_at else 1 for axis in range(result.ndim)]) for axis_at in (source, target)]
    chosen = jax.random.permutation(own_key, parts)[partner]
    strong = (owner == chosen) | (owner == (partner + parts // 2) % parts)
    return jnp.where(strong, factor * result, result)


def shard_levels(own_key, shape, cuts, smallest, top_value):
    level = 1.0
    for axis_at, parts in cuts:
        draws = jax.random.uniform(jax.random.fold_in(jax.random.fold_in(own_key, 6), axis_at), (parts,), jnp.float32, smallest / len(cuts), top_value / len(cuts))
        level = level * jnp.repeat(jnp.exp(draws), shape[axis_at] // parts).reshape((-1,) + (1,) * (len(shape) - 1 - axis_at))
    return level


def bell_draw(own_key, extent, deviation, bound, pieces=(), held_as=jnp.bfloat16):
    values = deviation * jax.random.normal(own_key, extent, jnp.float32)
    if pieces:
        values = values * shard_levels(own_key, extent, pieces, -0.22, 0.18)
    return jnp.clip(values, -bound, bound).astype(held_as)


def noise_with(own_key, dims, scale, most, cuts, heavy, dtype=jnp.bfloat16):
    entries = scale * jax.random.normal(own_key, dims, jnp.float32)
    if cuts:
        entries = entries * shard_levels(own_key, dims, cuts, -0.22, 0.18)
    return jnp.clip(with_spikes(entries, jax.random.fold_in(own_key, 3), *heavy), -most, most).astype(dtype)


def setup_inputs(seed: int = 0) -> dict:
    key_of = jax.random.split(jax.random.key(seed), 12)
    return {
        "hidden_in": bell_draw(key_of[0], (TOKENS, D), 1.0, 6.0, ((1, 4),)),
        "up_act": bell_draw(key_of[1], (TOKENS, FF), 1.0, 6.0, ((0, 4), (1, 8))),
        "up_val": bell_draw(key_of[2], (TOKENS, FF), 1.0, 6.0, ((0, 4), (1, 8))),
        "cotangent": noise_with(key_of[3], (TOKENS, D), 1.0, 6.0, ((0, 4),), (0, 1, 4, 2.0)),
        "w_act": bell_draw(key_of[4], (D, FF), D ** -0.5, 0.09375, ((0, 4), (1, 8))),
        "w_val": bell_draw(key_of[5], (D, FF), D ** -0.5, 0.09375, ((0, 4), (1, 8))),
        "w_down": bell_draw(key_of[6], (FF, D), FF ** -0.5, 0.0546875, ((0, 8), (1, 4))),
        "conv_act": bell_draw(key_of[7], (KW, FF), 0.577, 3.0, ((1, 8),)),
        "conv_val": bell_draw(key_of[8], (KW, FF), 0.577, 3.0, ((1, 8),)),
        "bias_act": bell_draw(key_of[9], (FF,), 0.5, 3.0, ((0, 8),)),
        "bias_val": bell_draw(key_of[10], (FF,), 0.5, 3.0, ((0, 8),)),
    }


def conv_ahead(upper, taps, bias):
    length = upper.shape[0]
    padded = jnp.concatenate([jnp.zeros((KW - 1, upper.shape[1]), jnp.float32), upper.astype(jnp.float32)], 0)
    total = jnp.zeros(upper.shape, jnp.float32) + bias.astype(jnp.float32)
    for offset in range(KW):
        total = total + taps[offset].astype(jnp.float32) * padded[offset:offset + length]
    return (total, padded)

def conv_behind(grad_pre, taps):
    length = grad_pre.shape[0]
    padded = jnp.concatenate([grad_pre, jnp.zeros((KW - 1, grad_pre.shape[1]), jnp.float32)], 0)
    total = jnp.zeros(grad_pre.shape, jnp.float32)
    for offset in range(KW):
        total = total + taps[offset].astype(jnp.float32) * padded[KW - 1 - offset:KW - 1 - offset + length]
    return total.astype(jnp.bfloat16)

def tap_grads(grad_pre, padded):
    length = grad_pre.shape[0]
    rows = [lax.optimization_barrier(jnp.sum(grad_pre * padded[offset:offset + length], axis=0)) for offset in range(KW)]
    return (jnp.stack(rows, 0), lax.optimization_barrier(jnp.sum(grad_pre, axis=0)))

def reference(hidden_in, up_act, up_val, cotangent, w_act, w_val, w_down, conv_act, conv_val, bias_act, bias_val):
    pre_act, padded_act = conv_ahead(up_act, conv_act, bias_act)
    pre_val, padded_val = conv_ahead(up_val, conv_val, bias_val)
    gelu_act, gelu_back = jax.vjp(jax.nn.gelu, pre_act)
    mixed = (gelu_act * pre_val).astype(jnp.bfloat16)
    grad_mixed = jnp.dot(cotangent, w_down.T, preferred_element_type=jnp.float32).astype(jnp.bfloat16)
    grad_mixed = lax.optimization_barrier(grad_mixed).astype(jnp.float32)
    grad_pre_act = gelu_back(grad_mixed * pre_val)[0]
    grad_pre_val = grad_mixed * gelu_act
    grad_up_act = conv_behind(grad_pre_act, conv_act)
    grad_up_val = conv_behind(grad_pre_val, conv_val)
    grad_conv_act, grad_bias_act = tap_grads(grad_pre_act, padded_act)
    grad_conv_val, grad_bias_val = tap_grads(grad_pre_val, padded_val)
    grad_w_act = jnp.dot(hidden_in.T, grad_up_act, preferred_element_type=jnp.float32)
    grad_w_val = jnp.dot(hidden_in.T, grad_up_val, preferred_element_type=jnp.float32)
    grad_w_down = jnp.dot(mixed.T, cotangent, preferred_element_type=jnp.float32)
    grad_input = jnp.dot(grad_up_act, w_act.T, preferred_element_type=jnp.float32)
    grad_input = grad_input + jnp.dot(grad_up_val, w_val.T, preferred_element_type=jnp.float32)
    grad_input = grad_input.astype(jnp.bfloat16)
    rows_act = lax.optimization_barrier(jnp.sum(grad_w_act * grad_w_act, axis=1))
    rows_val = lax.optimization_barrier(jnp.sum(grad_w_val * grad_w_val, axis=1))
    rows_down = lax.optimization_barrier(jnp.sum(grad_w_down * grad_w_down, axis=1))
    conv_rows = jnp.stack([lax.optimization_barrier(jnp.sum(grad_conv_act * grad_conv_act, axis=1)), lax.optimization_barrier(jnp.sum(grad_conv_val * grad_conv_val, axis=1))], 0)
    return (grad_input, grad_w_act, grad_w_val, grad_w_down, grad_conv_act, grad_conv_val, grad_bias_act, grad_bias_val, rows_act, rows_val, rows_down, conv_rows)
```

```python
import jax
import jax.numpy as jnp
from jax import lax
from jax.experimental import pallas as pl
from jax.experimental.pallas import tpu as pltpu
from jax.sharding import PartitionSpec as P

MESH = pl.DeviceIdType.MESH
F32 = jnp.float32
BF16 = jnp.bfloat16
CHUNK = 256
HALO = 16
TAIL = 8
ROOT_TWO_OVER_PI = 0.7978845608028654
CUBIC = 0.044715


def remote(copy_at, source, target, send, receive, where):
    return pltpu.make_async_remote_copy(
        src_ref=source,
        dst_ref=target,
        send_sem=send.at[copy_at],
        recv_sem=receive.at[copy_at],
        device_id=where,
        device_id_type=MESH,
    )


def greet(everyone):
    barrier = pltpu.get_barrier_semaphore()
    for where in everyone:
        pl.semaphore_signal(barrier, inc=1, device_id=where, device_id_type=MESH)
    pl.semaphore_wait(barrier, len(everyone))


def gradient_kernel(
    cot, down, up_a, up_v, taps_a, taps_v, bias_a, bias_v,
    columns, all_a, all_v, all_m, sums,
    own, to_sib, to_sib_far, to_far, from_sib, from_sib_far, from_far,
    before_a, before_v, grad_a, grad_v, after_a, after_v, own_sums, got_sums,
    send, receive,
):
    me = lax.axis_index("tp")
    count = lax.axis_size("tp")
    chip, core = me // 2, me % 2
    sib = chip * 2 + (1 - core)
    far = (1 - chip) * 2 + core
    diag = (1 - chip) * 2 + (1 - core)
    right, left = lax.rem(me + 1, count), lax.rem(me + count - 1, count)
    length, width = up_a.shape
    depth = down.shape[1]
    tap_count = taps_a.shape[0]
    reach = tap_count - 1

    def to(index):
        return {"tp": index}

    def rows(ref, index):
        return ref.at[pl.ds(pl.multiple_of(index * length, length), length), :]

    def cols(index):
        return pl.ds(pl.multiple_of(index * depth, depth), depth)

    greet([to(sib), to(far), to(diag)])
    cot_copies = [
        remote(slot, cot.at[:, cols(peer)], rows(columns, me), send, receive, to(peer))
        for slot, peer in ((0, sib), (1, far), (2, diag))
    ]
    last = pl.ds(length - HALO, HALO)
    halo_copies = [
        remote(3, up_a.at[last, :], before_a, send, receive, to(right)),
        remote(4, up_v.at[last, :], before_v, send, receive, to(right)),
    ]
    for copy in (cot_copies[1], cot_copies[2], cot_copies[0], *halo_copies):
        copy.start()
    rows(columns, me)[...] = cot[:, cols(me)]

    def partial(index, finish):
        block = rows(columns, index)[...]

        def step(at, carry):
            lanes = pl.ds(pl.multiple_of(at * CHUNK, CHUNK), CHUNK)
            finish(lanes, contract_last(block, down[lanes, :]))
            return carry

        lax.fori_loop(0, width // CHUNK, step, 0)

    def keep(target):
        def finish(lanes, value):
            target[:, lanes] = value.astype(target.dtype)

        return finish

    def add_far(lanes, value):
        to_far[:, lanes] = (value + from_sib_far[:, lanes].astype(F32)).astype(BF16)

    partial(me, keep(own))
    cot_copies[0].wait_recv()
    partial(sib, keep(to_sib))
    near_copy = remote(5, to_sib, from_sib, send, receive, to(sib))
    near_copy.start()
    cot_copies[2].wait_recv()
    partial(diag, keep(to_sib_far))
    relay_copy = remote(6, to_sib_far, from_sib_far, send, receive, to(sib))
    relay_copy.start()
    cot_copies[1].wait_recv()
    relay_copy.wait_recv()
    partial(far, add_far)
    far_copy = remote(7, to_far, from_far, send, receive, to(far))
    far_copy.start()
    for copy in halo_copies:
        copy.wait_recv()
    near_copy.wait_recv()
    far_copy.wait_recv()

    has_before = (me > 0).astype(F32)
    has_after = (me < count - 1).astype(F32)
    out_m, out_a, out_v = rows(all_m, me), rows(all_a, me), rows(all_v, me)

    def forward(at, carry):
        lanes = pl.ds(pl.multiple_of(at * CHUNK, CHUNK), CHUNK)
        ext_a = jnp.concatenate(
            [before_a[:, lanes].astype(F32) * has_before, up_a[:, lanes].astype(F32)], 0
        )
        ext_v = jnp.concatenate(
            [before_v[:, lanes].astype(F32) * has_before, up_v[:, lanes].astype(F32)], 0
        )
        taken_a = [ext_a[HALO - reach + k : HALO - reach + k + length] for k in range(tap_count)]
        taken_v = [ext_v[HALO - reach + k : HALO - reach + k + length] for k in range(tap_count)]
        pre_a = jnp.broadcast_to(bias_a[:, lanes].astype(F32), (length, CHUNK))
        pre_v = jnp.broadcast_to(bias_v[:, lanes].astype(F32), (length, CHUNK))
        for k in range(tap_count):
            pre_a = pre_a + taps_a[k : k + 1, lanes].astype(F32) * taken_a[k]
            pre_v = pre_v + taps_v[k : k + 1, lanes].astype(F32) * taken_v[k]
        square = pre_a * pre_a
        bent = jnp.tanh(ROOT_TWO_OVER_PI * pre_a * (1.0 + CUBIC * square))
        half = 0.5 * (1.0 + bent)
        gelu = pre_a * half
        slope = half + 0.5 * pre_a * (1.0 - bent * bent) * (
            ROOT_TWO_OVER_PI * (1.0 + 3.0 * CUBIC * square)
        )
        out_m[:, lanes] = (gelu * pre_v).astype(BF16)
        total = own[:, lanes] + from_sib[:, lanes].astype(F32) + from_far[:, lanes].astype(F32)
        grad_mixed = total.astype(BF16).astype(F32)
        pre_grad_a = grad_mixed * pre_v * slope
        pre_grad_v = grad_mixed * gelu
        grad_a[:, lanes] = pre_grad_a
        grad_v[:, lanes] = pre_grad_v
        found = [jnp.sum(pre_grad_a * taken, axis=0, keepdims=True) for taken in taken_a]
        found.append(jnp.sum(pre_grad_a, axis=0, keepdims=True))
        found += [jnp.sum(pre_grad_v * taken, axis=0, keepdims=True) for taken in taken_v]
        found.append(jnp.sum(pre_grad_v, axis=0, keepdims=True))
        own_sums[:, lanes] = jnp.concatenate(found, 0)
        return carry

    lax.fori_loop(0, width // CHUNK, forward, 0)
    first = pl.ds(0, TAIL)
    back_copies = [
        remote(8, grad_a.at[first, :], after_a, send, receive, to(left)),
        remote(9, grad_v.at[first, :], after_v, send, receive, to(left)),
    ]
    sum_copies = [
        remote(19 + slot, own_sums, got_sums.at[slot], send, receive, to(peer))
        for slot, peer in enumerate((sib, far, diag))
    ]

    def spread(slot, ref):
        pair = [
            remote(10 + slot, rows(ref, me), rows(ref, me), send, receive, to(far)),
            remote(13 + slot, rows(ref, me), rows(ref, me), send, receive, to(sib)),
        ]
        for copy in pair:
            copy.start()
        return pair

    for copy in back_copies:
        copy.start()
    spreads = [spread(0, all_m)]
    for copy in sum_copies:
        copy.start()

    def backward(grads, after, taps, out):
        def step(at, carry):
            lanes = pl.ds(pl.multiple_of(at * CHUNK, CHUNK), CHUNK)
            ext = jnp.concatenate([grads[:, lanes], after[:, lanes] * has_after], 0)
            total = jnp.zeros((length, CHUNK), F32)
            for k in range(tap_count):
                total = total + taps[k : k + 1, lanes].astype(F32) * ext[reach - k : reach - k + length]
            out[:, lanes] = total.astype(BF16)
            return carry

        lax.fori_loop(0, width // CHUNK, step, 0)

    back_copies[0].wait_recv()
    backward(grad_a, after_a, taps_a, out_a)
    spreads.append(spread(1, all_a))
    back_copies[1].wait_recv()
    backward(grad_v, after_v, taps_v, out_v)
    spreads.append(spread(2, all_v))
    relays = []
    for slot, (pair, ref) in enumerate(zip(spreads, (all_m, all_a, all_v))):
        pair[0].wait_recv()
        relay = remote(16 + slot, rows(ref, far), rows(ref, far), send, receive, to(sib))
        relay.start()
        relays.append(relay)
    for copy in sum_copies:
        copy.wait_recv()
    sums[...] = (own_sums[...] + got_sums[0]) + (got_sums[1] + got_sums[2])
    for pair, relay in zip(spreads, relays):
        pair[1].wait_recv()
        relay.wait_recv()
    for copy in (
        *cot_copies, *halo_copies, near_copy, relay_copy, far_copy, *back_copies, *sum_copies,
        *(copy for pair in spreads for copy in pair), *relays,
    ):
        copy.wait_send()


def gradients(cotangent, w_down, up_act, up_val, conv_act, conv_val, bias_act, bias_val):
    length, width = up_act.shape
    depth = w_down.shape[1]
    tp_count = lax.axis_size("tp")
    tap_count = conv_act.shape[0]
    positions = length * tp_count
    stat_rows = 2 * (tap_count + 1)
    vmem = pl.BlockSpec(memory_space=pltpu.VMEM)
    block = pltpu.VMEM((length, width), BF16)
    wide = pltpu.VMEM((length, width), F32)
    return pl.pallas_call(
        gradient_kernel,
        out_shape=(
            jax.ShapeDtypeStruct((positions, depth), BF16),
            jax.ShapeDtypeStruct((positions, width), BF16),
            jax.ShapeDtypeStruct((positions, width), BF16),
            jax.ShapeDtypeStruct((positions, width), BF16),
            jax.ShapeDtypeStruct((stat_rows, width), F32),
        ),
        in_specs=[vmem] * 8,
        out_specs=(vmem,) * 5,
        scratch_shapes=[
            wide, block, block, block, block, block, block,
            pltpu.VMEM((HALO, width), BF16), pltpu.VMEM((HALO, width), BF16),
            wide, wide,
            pltpu.VMEM((TAIL, width), F32), pltpu.VMEM((TAIL, width), F32),
            pltpu.VMEM((stat_rows, width), F32), pltpu.VMEM((3, stat_rows, width), F32),
            pltpu.SemaphoreType.DMA((22,)), pltpu.SemaphoreType.DMA((22,)),
        ],
        compiler_params=pltpu.CompilerParams(
            collective_id=0, has_side_effects=True, vmem_limit_bytes=50 * 1024 * 1024
        ),
    )(
        cotangent, w_down, up_act, up_val, conv_act, conv_val,
        bias_act.reshape(1, width), bias_val.reshape(1, width),
    )


def reduce_kernel(
    terms, stat, down_stat, out, stat_sum, down_sum,
    to_pair, from_pair, to_line, from_line, settled, got_stat, got_down,
    send, receive,
):
    fs, tp = lax.axis_index("fs"), lax.axis_index("tp")
    fs_count, tp_count = lax.axis_size("fs"), lax.axis_size("tp")
    line = fs_count // 2
    z, y = fs // 2, fs % 2
    pair = z * 2 + (1 - y)
    shard = out.shape[0]
    depth = terms.shape[1]
    length = terms.shape[0] // tp_count

    def at_fs(index):
        return {"fs": index}

    def at_tp(index):
        return {"tp": index}

    fs_others = [lax.rem(fs + by, fs_count) for by in range(1, fs_count)]
    tp_others = [lax.rem(tp + by, tp_count) for by in range(1, tp_count)]
    greet([at_fs(i) for i in fs_others] + [at_tp(i) for i in tp_others])

    def term(index):
        return jnp.concatenate(
            [
                terms[pl.ds(pl.multiple_of(part * length + index * shard, shard), shard), :]
                for part in range(tp_count)
            ],
            0,
        )

    base = 0
    steps = sorted(range(1, line), key=lambda by: -min(by, line - by)) + [0]
    there = {by: lax.rem(z + by, line) for by in steps}
    pair_copies = {}
    for by in steps:
        to_pair[by] = term(there[by] * 2 + (1 - y)).astype(BF16)
        pair_copies[by] = remote(
            base + by, to_pair.at[by], from_pair.at[by], send, receive, at_fs(pair)
        )
        pair_copies[by].start()
    base += line
    small = []
    for slot, index in enumerate(fs_others):
        small.append(remote(base + slot, stat, got_stat.at[slot], send, receive, at_fs(index)))
    base += len(fs_others)
    for slot, index in enumerate(tp_others):
        small.append(
            remote(base + slot, down_stat, got_down.at[slot], send, receive, at_tp(index))
        )
    base += len(tp_others)
    for copy in small:
        copy.start()
    line_copies = []
    total = None
    for by in steps:
        pair_copies[by].wait_recv()
        added = term(there[by] * 2 + y) + from_pair[by].astype(F32)
        if by == 0:
            total = added
        else:
            to_line[by] = added.astype(BF16)
            copy = remote(
                base + by, to_line.at[by], from_line.at[by], send, receive,
                at_fs(there[by] * 2 + y),
            )
            copy.start()
            line_copies.append((by, copy))
    base += line
    for by, copy in line_copies:
        copy.wait_recv()
        total = total + from_line[by].astype(F32)
    settled[...] = total.astype(BF16)

    def part_of(index):
        return pl.ds(pl.multiple_of(index * shard, shard), shard)

    mine = pl.ds(pl.multiple_of(tp * depth, depth), depth)
    last_copies = [
        remote(
            base + slot, settled.at[part_of(index), :], out.at[:, mine], send, receive, at_tp(index)
        )
        for slot, index in enumerate(tp_others)
    ]
    for copy in last_copies:
        copy.start()
    out[:, mine] = settled[part_of(tp), :]
    for copy in small:
        copy.wait_recv()
    stat_total = stat[...]
    for slot in range(len(fs_others)):
        stat_total = stat_total + got_stat[slot]
    stat_sum[...] = stat_total
    down_total = down_stat[...]
    for slot in range(len(tp_others)):
        down_total = down_total + got_down[slot]
    down_sum[...] = down_total
    for copy in last_copies:
        copy.wait_recv()
    for copy in (
        *pair_copies.values(), *small, *(copy for _, copy in line_copies), *last_copies,
    ):
        copy.wait_send()


def reduced(terms, stat, down_stat):
    fs_count, tp_count = lax.axis_size("fs"), lax.axis_size("tp")
    positions, depth = terms.shape
    shard = positions // (fs_count * tp_count)
    line = fs_count // 2
    vmem = pl.BlockSpec(memory_space=pltpu.VMEM)
    blocks = pltpu.VMEM((line, tp_count * shard, depth), BF16)
    copies = 2 * line + (fs_count - 1) + 2 * (tp_count - 1)
    return pl.pallas_call(
        reduce_kernel,
        out_shape=(
            jax.ShapeDtypeStruct((shard, depth * tp_count), BF16),
            jax.ShapeDtypeStruct(stat.shape, F32),
            jax.ShapeDtypeStruct(down_stat.shape, F32),
        ),
        in_specs=[vmem] * 3,
        out_specs=(vmem,) * 3,
        scratch_shapes=[
            blocks, blocks, blocks, blocks,
            pltpu.VMEM((tp_count * shard, depth), BF16),
            pltpu.VMEM((fs_count - 1,) + stat.shape, F32),
            pltpu.VMEM((tp_count - 1,) + down_stat.shape, F32),
            pltpu.SemaphoreType.DMA((copies,)), pltpu.SemaphoreType.DMA((copies,)),
        ],
        compiler_params=pltpu.CompilerParams(collective_id=1, has_side_effects=True),
    )(terms, stat, down_stat)


def kernels_fit(up_act, w_down, conv_act):
    length, width = up_act.shape
    fs_count, tp_count = lax.axis_size("fs"), lax.axis_size("tp")
    return (
        tp_count == 4
        and fs_count % 2 == 0
        and width % CHUNK == 0
        and w_down.shape[1] % 128 == 0
        and length % (16 * fs_count) == 0
        and conv_act.shape[0] - 1 <= TAIL
        and conv_act.shape[0] == 3
        and width * (w_down.shape[1] + 24 * length) * 2 <= 24 * 1024 * 1024
    )


def with_kernels(
    hidden_in, up_act, up_val, cotangent, w_act, w_val, w_down,
    conv_act, conv_val, bias_act, bias_val,
):
    tap_count = conv_act.shape[0]
    cot_columns, all_up_act, all_up_val, all_mixed, sums = gradients(
        cotangent, w_down, up_act, up_val, conv_act, conv_val, bias_act, bias_val
    )
    grad_w_act = contract_first(hidden_in, all_up_act)
    grad_w_val = contract_first(hidden_in, all_up_val)
    grad_w_down = contract_first(all_mixed, cot_columns)
    terms = contract_last(all_up_act, w_act) + contract_last(all_up_val, w_val)
    taps_act, sums_act = sums[:tap_count], sums[tap_count]
    taps_val, sums_val = sums[tap_count + 1 : 2 * tap_count + 1], sums[2 * tap_count + 1]
    tap_squares = jnp.stack(
        [jnp.sum(taps_act * taps_act, axis=1), jnp.sum(taps_val * taps_val, axis=1)], 0
    )
    depth = hidden_in.shape[1]
    flat = tap_squares.reshape(1, -1)
    stat = jnp.concatenate(
        [
            jnp.sum(grad_w_act * grad_w_act, axis=1)[None],
            jnp.sum(grad_w_val * grad_w_val, axis=1)[None],
            jnp.pad(flat, ((0, 0), (0, depth - flat.shape[1]))),
            jnp.zeros((5, depth), F32),
        ],
        0,
    )
    down_stat = jnp.pad(jnp.sum(grad_w_down * grad_w_down, axis=1)[None], ((0, 7), (0, 0)))
    grad_input, stat, down_stat = reduced(terms, stat, down_stat)
    return (
        grad_input,
        grad_w_act,
        grad_w_val,
        grad_w_down,
        taps_act,
        taps_val,
        sums_act,
        sums_val,
        stat[0],
        stat[1],
        down_stat[0],
        stat[2, : 2 * tap_count].reshape(2, tap_count),
    )


def passed_along(value, axis, by):
    length = lax.axis_size(axis)
    pairs = [(i, i + by) for i in range(length) if 0 <= i + by < length]
    return lax.ppermute(value, axis, pairs)


def contract_last(left, right):
    return lax.dot_general(
        left, right, (((1,), (1,)), ((), ())), preferred_element_type=jnp.float32
    )


def contract_first(left, right):
    return lax.dot_general(
        left, right, (((0,), (0,)), ((), ())), preferred_element_type=jnp.float32
    )


def conv_ahead(extended, taps, bias, length):
    total = jnp.zeros((length, extended.shape[1]), jnp.float32) + bias.astype(jnp.float32)
    for offset in range(taps.shape[0]):
        total = total + taps[offset].astype(jnp.float32) * extended[offset : offset + length]
    return total


def conv_behind(extended, taps, length):
    reach = taps.shape[0] - 1
    total = jnp.zeros((length, extended.shape[1]), jnp.float32)
    for offset in range(taps.shape[0]):
        total = (
            total
            + taps[offset].astype(jnp.float32) * extended[reach - offset : reach - offset + length]
        )
    return total.astype(jnp.bfloat16)


def tap_grads(grad_pre, extended, tap_count):
    length = grad_pre.shape[0]
    rows = [
        jnp.sum(grad_pre * extended[offset : offset + length], axis=0)
        for offset in range(tap_count)
    ]
    return (jnp.stack(rows, 0), jnp.sum(grad_pre, axis=0))


def per_device(
    hidden_in,
    up_act,
    up_val,
    cotangent,
    w_act,
    w_val,
    w_down,
    conv_act,
    conv_val,
    bias_act,
    bias_val,
):
    if kernels_fit(up_act, w_down, conv_act):
        return with_kernels(
            hidden_in, up_act, up_val, cotangent, w_act, w_val, w_down,
            conv_act, conv_val, bias_act, bias_val,
        )
    local_rows = cotangent.shape[0]
    tap_count = conv_act.shape[0]
    reach = tap_count - 1
    tp_count = lax.axis_size("tp")
    fs_count = lax.axis_size("fs")
    down_whole = lax.all_gather(w_down, "tp", axis=1, tiled=True)
    prev_act, prev_val = passed_along(
        (up_act[local_rows - reach :], up_val[local_rows - reach :]), "tp", 1
    )
    ext_act = jnp.concatenate([prev_act, up_act], 0).astype(jnp.float32)
    ext_val = jnp.concatenate([prev_val, up_val], 0).astype(jnp.float32)
    pre_act = conv_ahead(ext_act, conv_act, bias_act, local_rows)
    pre_val = conv_ahead(ext_val, conv_val, bias_val, local_rows)
    gelu_act, gelu_back = jax.vjp(jax.nn.gelu, pre_act)
    mixed = (gelu_act * pre_val).astype(jnp.bfloat16)
    grad_mixed = contract_last(cotangent, down_whole).astype(jnp.bfloat16)
    grad_mixed = lax.optimization_barrier(grad_mixed).astype(jnp.float32)
    grad_pre_act = gelu_back(grad_mixed * pre_val)[0]
    grad_pre_val = grad_mixed * gelu_act
    next_act, next_val = passed_along((grad_pre_act[:reach], grad_pre_val[:reach]), "tp", -1)
    grad_up_act = conv_behind(jnp.concatenate([grad_pre_act, next_act], 0), conv_act, local_rows)
    grad_up_val = conv_behind(jnp.concatenate([grad_pre_val, next_val], 0), conv_val, local_rows)
    taps_act, sums_act = tap_grads(grad_pre_act, ext_act, tap_count)
    taps_val, sums_val = tap_grads(grad_pre_val, ext_val, tap_count)
    all_up_act, all_up_val, all_mixed = (
        lax.all_gather(grad_up_act, "tp", axis=0, tiled=True),
        lax.all_gather(grad_up_val, "tp", axis=0, tiled=True),
        lax.all_gather(mixed, "tp", axis=0, tiled=True),
    )
    cot_columns = lax.all_to_all(cotangent, "tp", split_axis=1, concat_axis=0, tiled=True)
    grad_w_act = contract_first(hidden_in, all_up_act)
    grad_w_val = contract_first(hidden_in, all_up_val)
    grad_w_down = contract_first(all_mixed, cot_columns)
    shard_rows = local_rows // fs_count
    block_rows = tp_count * shard_rows

    def select_rows(gathered):
        shaped = gathered.reshape(tp_count, fs_count, shard_rows, gathered.shape[1])
        return jnp.transpose(shaped, (1, 0, 2, 3)).reshape(
            lax.axis_size("fs") * block_rows, gathered.shape[1]
        )

    summed = lax.psum_scatter(
        contract_last(select_rows(all_up_act), w_act)
        + contract_last(select_rows(all_up_val), w_val),
        "fs",
        scatter_dimension=0,
        tiled=True,
    ).astype(jnp.bfloat16)
    grad_input = lax.all_to_all(summed, "tp", split_axis=0, concat_axis=1, tiled=True)
    down_squares = jnp.sum(grad_w_down * grad_w_down, axis=1)
    taps_act, taps_val, sums_act, sums_val, rows_down = lax.psum(
        (taps_act, taps_val, sums_act, sums_val, down_squares), "tp"
    )
    tap_squares = jnp.stack(
        [jnp.sum(taps_act * taps_act, axis=1), jnp.sum(taps_val * taps_val, axis=1)], 0
    )
    rows_act, rows_val, conv_rows = lax.psum(
        (
            jnp.sum(grad_w_act * grad_w_act, axis=1),
            jnp.sum(grad_w_val * grad_w_val, axis=1),
            tap_squares,
        ),
        "fs",
    )
    return (
        grad_input,
        grad_w_act,
        grad_w_val,
        grad_w_down,
        taps_act,
        taps_val,
        sums_act,
        sums_val,
        rows_act,
        rows_val,
        rows_down,
        conv_rows,
    )


def solution(mesh):
    return jax.shard_map(
        per_device,
        mesh=mesh,
        in_specs=(
            P(None, "tp"),
            P("tp", "fs"),
            P("tp", "fs"),
            P("tp", None),
            P("tp", "fs"),
            P("tp", "fs"),
            P("fs", "tp"),
            P(None, "fs"),
            P(None, "fs"),
            P("fs"),
            P("fs"),
        ),
        out_specs=(
            P(("tp", "fs"), None),
            P("tp", "fs"),
            P("tp", "fs"),
            P("fs", "tp"),
            P(None, "fs"),
            P(None, "fs"),
            P("fs"),
            P("fs"),
            P("tp"),
            P("tp"),
            P("fs"),
            P(),
        ),
        check_vma=False,
    )
```

```python
import jax
import jax.numpy as jnp
from jax import lax
from jax.experimental import pallas as pl
from jax.experimental.pallas import tpu as pltpu
from jax.sharding import PartitionSpec as P

MESH = pl.DeviceIdType.MESH
F32 = jnp.float32
BF16 = jnp.bfloat16
CHUNK = 256
HALO = 16
TAIL = 8
ROOT_TWO_OVER_PI = 0.7978845608028654
CUBIC = 0.044715


def remote(copy_at, source, target, send, receive, where):
    return pltpu.make_async_remote_copy(
        src_ref=source,
        dst_ref=target,
        send_sem=send.at[copy_at],
        recv_sem=receive.at[copy_at],
        device_id=where,
        device_id_type=MESH,
    )


def greet(everyone):
    barrier = pltpu.get_barrier_semaphore()
    for where in everyone:
        pl.semaphore_signal(barrier, inc=1, device_id=where, device_id_type=MESH)
    pl.semaphore_wait(barrier, len(everyone))


def gradient_kernel(
    cot, down, up_a, up_v, taps_a, taps_v, bias_a, bias_v, weights_a, weights_v,
    columns, all_a, all_v, all_m, sums, terms,
    own, to_sib, to_sib_far, to_far, from_sib, from_sib_far, from_far,
    before_a, before_v, grad_a, grad_v, after_a, after_v, own_sums, got_sums,
    gated, factor, held_a, held_v,
    send, receive, loaded,
):
    me = lax.axis_index("tp")
    count = lax.axis_size("tp")
    chip, core = me // 2, me % 2
    sib = chip * 2 + (1 - core)
    far = (1 - chip) * 2 + core
    diag = (1 - chip) * 2 + (1 - core)
    right, left = lax.rem(me + 1, count), lax.rem(me + count - 1, count)
    length, width = up_a.shape
    depth = down.shape[1]
    tap_count = taps_a.shape[0]
    reach = tap_count - 1

    def to(index):
        return {"tp": index}

    def rows(ref, index):
        return ref.at[pl.ds(pl.multiple_of(index * length, length), length), :]

    def cols(index):
        return pl.ds(pl.multiple_of(index * depth, depth), depth)

    loads = [
        pltpu.make_async_copy(weights_a, held_a, loaded.at[0]),
        pltpu.make_async_copy(weights_v, held_v, loaded.at[1]),
    ]
    for load in loads:
        load.start()
    greet([to(sib), to(far), to(diag)])
    cot_copies = [
        remote(slot, cot.at[:, cols(peer)], rows(columns, me), send, receive, to(peer))
        for slot, peer in ((0, sib), (1, far), (2, diag))
    ]
    last = pl.ds(length - HALO, HALO)
    halo_copies = [
        remote(3, up_a.at[last, :], before_a, send, receive, to(right)),
        remote(4, up_v.at[last, :], before_v, send, receive, to(right)),
    ]
    for copy in (cot_copies[1], cot_copies[2], cot_copies[0], *halo_copies):
        copy.start()
    rows(columns, me)[...] = cot[:, cols(me)]

    def partial(index, finish):
        block = rows(columns, index)[...]

        def step(at, carry):
            lanes = pl.ds(pl.multiple_of(at * CHUNK, CHUNK), CHUNK)
            finish(lanes, contract_last(block, down[lanes, :]))
            return carry

        lax.fori_loop(0, width // CHUNK, step, 0)

    def keep(target):
        def finish(lanes, value):
            target[:, lanes] = value.astype(target.dtype)

        return finish

    def add_far(lanes, value):
        to_far[:, lanes] = (value + from_sib_far[:, lanes].astype(F32)).astype(BF16)

    has_before = (me > 0).astype(F32)
    has_after = (me < count - 1).astype(F32)
    out_m, out_a, out_v = rows(all_m, me), rows(all_a, me), rows(all_v, me)

    def shifted(before, up, lanes):
        ext = jnp.concatenate(
            [before[:, lanes].astype(F32) * has_before, up[:, lanes].astype(F32)], 0
        )
        return [ext[HALO - reach + k : HALO - reach + k + length] for k in range(tap_count)]

    def forward(at, carry):
        lanes = pl.ds(pl.multiple_of(at * CHUNK, CHUNK), CHUNK)
        taken_a, taken_v = shifted(before_a, up_a, lanes), shifted(before_v, up_v, lanes)
        pre_a = jnp.broadcast_to(bias_a[:, lanes].astype(F32), (length, CHUNK))
        pre_v = jnp.broadcast_to(bias_v[:, lanes].astype(F32), (length, CHUNK))
        for k in range(tap_count):
            pre_a = pre_a + taps_a[k : k + 1, lanes].astype(F32) * taken_a[k]
            pre_v = pre_v + taps_v[k : k + 1, lanes].astype(F32) * taken_v[k]
        square = pre_a * pre_a
        bent = jnp.tanh(ROOT_TWO_OVER_PI * pre_a * (1.0 + CUBIC * square))
        half = 0.5 * (1.0 + bent)
        gelu = pre_a * half
        slope = half + 0.5 * pre_a * (1.0 - bent * bent) * (
            ROOT_TWO_OVER_PI * (1.0 + 3.0 * CUBIC * square)
        )
        out_m[:, lanes] = (gelu * pre_v).astype(BF16)
        gated[:, lanes] = gelu
        factor[:, lanes] = pre_v * slope
        return carry

    def spread(slot, ref):
        pair = [
            remote(10 + slot, rows(ref, me), rows(ref, me), send, receive, to(far)),
            remote(13 + slot, rows(ref, me), rows(ref, me), send, receive, to(sib)),
        ]
        for copy in pair:
            copy.start()
        return pair

    partial(me, keep(own))
    for copy in halo_copies:
        copy.wait_recv()
    lax.fori_loop(0, width // CHUNK, forward, 0)
    spreads = [spread(0, all_m)]
    cot_copies[0].wait_recv()
    partial(sib, keep(to_sib))
    near_copy = remote(5, to_sib, from_sib, send, receive, to(sib))
    near_copy.start()
    cot_copies[2].wait_recv()
    partial(diag, keep(to_sib_far))
    relay_copy = remote(6, to_sib_far, from_sib_far, send, receive, to(sib))
    relay_copy.start()
    cot_copies[1].wait_recv()
    relay_copy.wait_recv()
    partial(far, add_far)
    far_copy = remote(7, to_far, from_far, send, receive, to(far))
    far_copy.start()
    relays = []

    def relay_rows(slot, ref):
        spreads[slot][0].wait_recv()
        copy = remote(16 + slot, rows(ref, far), rows(ref, far), send, receive, to(sib))
        copy.start()
        relays.append(copy)

    relay_rows(0, all_m)
    near_copy.wait_recv()
    far_copy.wait_recv()


    def combine(at, carry):
        lanes = pl.ds(pl.multiple_of(at * CHUNK, CHUNK), CHUNK)
        taken_a, taken_v = shifted(before_a, up_a, lanes), shifted(before_v, up_v, lanes)
        total = own[:, lanes] + from_sib[:, lanes].astype(F32) + from_far[:, lanes].astype(F32)
        grad_mixed = total.astype(BF16).astype(F32)
        pre_grad_a = grad_mixed * factor[:, lanes]
        pre_grad_v = grad_mixed * gated[:, lanes]
        grad_a[:, lanes] = pre_grad_a
        grad_v[:, lanes] = pre_grad_v
        found = [jnp.sum(pre_grad_a * taken, axis=0, keepdims=True) for taken in taken_a]
        found.append(jnp.sum(pre_grad_a, axis=0, keepdims=True))
        found += [jnp.sum(pre_grad_v * taken, axis=0, keepdims=True) for taken in taken_v]
        found.append(jnp.sum(pre_grad_v, axis=0, keepdims=True))
        own_sums[:, lanes] = jnp.concatenate(found, 0)
        return carry

    lax.fori_loop(0, width // CHUNK, combine, 0)
    first = pl.ds(0, TAIL)
    back_copies = [
        remote(8, grad_a.at[first, :], after_a, send, receive, to(left)),
        remote(9, grad_v.at[first, :], after_v, send, receive, to(left)),
    ]
    sum_copies = [
        remote(19 + slot, own_sums, got_sums.at[slot], send, receive, to(peer))
        for slot, peer in enumerate((sib, far, diag))
    ]

    for copy in back_copies:
        copy.start()
    for copy in sum_copies:
        copy.start()

    def backward(grads, after, taps, out):
        def step(at, carry):
            lanes = pl.ds(pl.multiple_of(at * CHUNK, CHUNK), CHUNK)
            ext = jnp.concatenate([grads[:, lanes], after[:, lanes] * has_after], 0)
            total = jnp.zeros((length, CHUNK), F32)
            for k in range(tap_count):
                total = total + taps[k : k + 1, lanes].astype(F32) * ext[reach - k : reach - k + length]
            out[:, lanes] = total.astype(BF16)
            return carry

        lax.fori_loop(0, width // CHUNK, step, 0)

    back_copies[0].wait_recv()
    backward(grad_a, after_a, taps_a, out_a)
    spreads.append(spread(1, all_a))
    back_copies[1].wait_recv()
    backward(grad_v, after_v, taps_v, out_v)
    spreads.append(spread(2, all_v))

    def add_terms(index, pairs, fresh):
        span = pl.ds(pl.multiple_of(index * length, length), length)

        def step(at, carry):
            lanes = pl.ds(pl.multiple_of(at * CHUNK, CHUNK), CHUNK)
            total = None if fresh else terms[span, lanes]
            for ref, weights in pairs:
                product = contract_last(ref[span, :], weights[lanes, :])
                total = product if total is None else total + product
            terms[span, lanes] = total
            return carry

        lax.fori_loop(0, depth // CHUNK, step, 0)

    role_a, role_v = (all_a, held_a), (all_v, held_v)
    for load in loads:
        load.wait()
    add_terms(me, (role_a, role_v), True)
    spreads[1][1].wait_recv()
    spreads[2][1].wait_recv()
    add_terms(sib, (role_a, role_v), True)
    relay_rows(1, all_a)
    add_terms(far, (role_a,), True)
    relays[1].wait_recv()
    add_terms(diag, (role_a,), True)
    relay_rows(2, all_v)
    add_terms(far, (role_v,), False)
    relays[2].wait_recv()
    add_terms(diag, (role_v,), False)
    for copy in sum_copies:
        copy.wait_recv()
    sums[...] = (own_sums[...] + got_sums[0]) + (got_sums[1] + got_sums[2])
    spreads[0][1].wait_recv()
    relays[0].wait_recv()
    for copy in (
        *cot_copies, *halo_copies, near_copy, relay_copy, far_copy, *back_copies, *sum_copies,
        *(copy for pair in spreads for copy in pair), *relays,
    ):
        copy.wait_send()


def gradients(
    cotangent, w_down, up_act, up_val, conv_act, conv_val, bias_act, bias_val, w_act, w_val
):
    length, width = up_act.shape
    depth = w_down.shape[1]
    tp_count = lax.axis_size("tp")
    tap_count = conv_act.shape[0]
    positions = length * tp_count
    stat_rows = 2 * (tap_count + 1)
    vmem = pl.BlockSpec(memory_space=pltpu.VMEM)
    block = pltpu.VMEM((length, width), BF16)
    wide = pltpu.VMEM((length, width), F32)
    return pl.pallas_call(
        gradient_kernel,
        out_shape=(
            jax.ShapeDtypeStruct((positions, depth), BF16),
            jax.ShapeDtypeStruct((positions, width), BF16),
            jax.ShapeDtypeStruct((positions, width), BF16),
            jax.ShapeDtypeStruct((positions, width), BF16),
            jax.ShapeDtypeStruct((stat_rows, width), F32),
            jax.ShapeDtypeStruct((positions, depth), F32),
        ),
        in_specs=[vmem] * 8 + [pl.BlockSpec(memory_space=pl.ANY)] * 2,
        out_specs=(vmem,) * 6,
        scratch_shapes=[
            wide, block, block, block, block, block, block,
            pltpu.VMEM((HALO, width), BF16), pltpu.VMEM((HALO, width), BF16),
            wide, wide,
            pltpu.VMEM((TAIL, width), F32), pltpu.VMEM((TAIL, width), F32),
            pltpu.VMEM((stat_rows, width), F32), pltpu.VMEM((3, stat_rows, width), F32),
            wide, wide, pltpu.VMEM(w_act.shape, BF16), pltpu.VMEM(w_val.shape, BF16),
            pltpu.SemaphoreType.DMA((22,)), pltpu.SemaphoreType.DMA((22,)),
            pltpu.SemaphoreType.DMA((2,)),
        ],
        compiler_params=pltpu.CompilerParams(
            collective_id=0, has_side_effects=True, vmem_limit_bytes=50 * 1024 * 1024
        ),
    )(
        cotangent, w_down, up_act, up_val, conv_act, conv_val,
        bias_act.reshape(1, width), bias_val.reshape(1, width), w_act, w_val,
    )


def reduce_kernel(
    terms, stat, down_stat, out, stat_sum, down_sum,
    to_pair, from_pair, to_line, from_line, settled, got_stat, got_down,
    send, receive,
):
    fs, tp = lax.axis_index("fs"), lax.axis_index("tp")
    fs_count, tp_count = lax.axis_size("fs"), lax.axis_size("tp")
    line = fs_count // 2
    z, y = fs // 2, fs % 2
    pair = z * 2 + (1 - y)
    shard = out.shape[0]
    depth = terms.shape[1]
    length = terms.shape[0] // tp_count

    def at_fs(index):
        return {"fs": index}

    def at_tp(index):
        return {"tp": index}

    fs_others = [lax.rem(fs + by, fs_count) for by in range(1, fs_count)]
    tp_others = [lax.rem(tp + by, tp_count) for by in range(1, tp_count)]
    greet([at_fs(i) for i in fs_others] + [at_tp(i) for i in tp_others])

    def term(index):
        return jnp.concatenate(
            [
                terms[pl.ds(pl.multiple_of(part * length + index * shard, shard), shard), :]
                for part in range(tp_count)
            ],
            0,
        )

    base = 0
    steps = sorted(range(1, line), key=lambda by: -min(by, line - by)) + [0]
    there = {by: lax.rem(z + by, line) for by in steps}
    pair_copies = {}
    for by in steps:
        to_pair[by] = term(there[by] * 2 + (1 - y)).astype(BF16)
        pair_copies[by] = remote(
            base + by, to_pair.at[by], from_pair.at[by], send, receive, at_fs(pair)
        )
        pair_copies[by].start()
    base += line
    small = []
    for slot, index in enumerate(fs_others):
        small.append(remote(base + slot, stat, got_stat.at[slot], send, receive, at_fs(index)))
    base += len(fs_others)
    for slot, index in enumerate(tp_others):
        small.append(
            remote(base + slot, down_stat, got_down.at[slot], send, receive, at_tp(index))
        )
    base += len(tp_others)
    for copy in small:
        copy.start()
    line_copies = []
    total = None
    for by in steps:
        pair_copies[by].wait_recv()
        added = term(there[by] * 2 + y) + from_pair[by].astype(F32)
        if by == 0:
            total = added
        else:
            to_line[by] = added.astype(BF16)
            copy = remote(
                base + by, to_line.at[by], from_line.at[by], send, receive,
                at_fs(there[by] * 2 + y),
            )
            copy.start()
            line_copies.append((by, copy))
    base += line
    for by, copy in line_copies:
        copy.wait_recv()
        total = total + from_line[by].astype(F32)
    settled[...] = total.astype(BF16)

    def part_of(index):
        return pl.ds(pl.multiple_of(index * shard, shard), shard)

    mine = pl.ds(pl.multiple_of(tp * depth, depth), depth)
    last_copies = [
        remote(
            base + slot, settled.at[part_of(index), :], out.at[:, mine], send, receive, at_tp(index)
        )
        for slot, index in enumerate(tp_others)
    ]
    for copy in last_copies:
        copy.start()
    out[:, mine] = settled[part_of(tp), :]
    for copy in small:
        copy.wait_recv()
    stat_total = stat[...]
    for slot in range(len(fs_others)):
        stat_total = stat_total + got_stat[slot]
    stat_sum[...] = stat_total
    down_total = down_stat[...]
    for slot in range(len(tp_others)):
        down_total = down_total + got_down[slot]
    down_sum[...] = down_total
    for copy in last_copies:
        copy.wait_recv()
    for copy in (
        *pair_copies.values(), *small, *(copy for _, copy in line_copies), *last_copies,
    ):
        copy.wait_send()


def reduced(terms, stat, down_stat):
    fs_count, tp_count = lax.axis_size("fs"), lax.axis_size("tp")
    positions, depth = terms.shape
    shard = positions // (fs_count * tp_count)
    line = fs_count // 2
    vmem = pl.BlockSpec(memory_space=pltpu.VMEM)
    blocks = pltpu.VMEM((line, tp_count * shard, depth), BF16)
    copies = 2 * line + (fs_count - 1) + 2 * (tp_count - 1)
    return pl.pallas_call(
        reduce_kernel,
        out_shape=(
            jax.ShapeDtypeStruct((shard, depth * tp_count), BF16),
            jax.ShapeDtypeStruct(stat.shape, F32),
            jax.ShapeDtypeStruct(down_stat.shape, F32),
        ),
        in_specs=[vmem] * 3,
        out_specs=(vmem,) * 3,
        scratch_shapes=[
            blocks, blocks, blocks, blocks,
            pltpu.VMEM((tp_count * shard, depth), BF16),
            pltpu.VMEM((fs_count - 1,) + stat.shape, F32),
            pltpu.VMEM((tp_count - 1,) + down_stat.shape, F32),
            pltpu.SemaphoreType.DMA((copies,)), pltpu.SemaphoreType.DMA((copies,)),
        ],
        compiler_params=pltpu.CompilerParams(collective_id=1, has_side_effects=True),
    )(terms, stat, down_stat)


def kernels_fit(up_act, w_down, conv_act):
    length, width = up_act.shape
    fs_count, tp_count = lax.axis_size("fs"), lax.axis_size("tp")
    return (
        tp_count == 4
        and fs_count % 2 == 0
        and width % CHUNK == 0
        and w_down.shape[1] % CHUNK == 0
        and length % (16 * fs_count) == 0
        and conv_act.shape[0] - 1 <= TAIL
        and conv_act.shape[0] == 3
        and width * (3 * w_down.shape[1] + 32 * length) * 2 <= 32 * 1024 * 1024
    )


def weight_kernel(left, right, out, norms):
    value = contract_first(left[...], right[...])
    out[...] = value
    square = value * value
    lanes = square[:, :128]
    for at in range(128, square.shape[1], 128):
        lanes = lanes + square[:, at : at + 128]
    norms[...] = jnp.sum(lanes.T, axis=0, keepdims=True)


def weight_gradient(left, right):
    positions, height = left.shape
    width = right.shape[1]
    return pl.pallas_call(
        weight_kernel,
        grid=(height // CHUNK,),
        out_shape=(
            jax.ShapeDtypeStruct((height, width), F32),
            jax.ShapeDtypeStruct((1, height), F32),
        ),
        in_specs=[
            pl.BlockSpec((positions, CHUNK), lambda i: (0, i)),
            pl.BlockSpec((positions, width), lambda i: (0, 0)),
        ],
        out_specs=(
            pl.BlockSpec((CHUNK, width), lambda i: (i, 0)),
            pl.BlockSpec((1, CHUNK), lambda i: (0, i)),
        ),
        compiler_params=pltpu.CompilerParams(vmem_limit_bytes=40 * 1024 * 1024),
    )(left, right)


def with_kernels(
    hidden_in, up_act, up_val, cotangent, w_act, w_val, w_down,
    conv_act, conv_val, bias_act, bias_val,
):
    tap_count = conv_act.shape[0]
    cot_columns, all_up_act, all_up_val, all_mixed, sums, terms = gradients(
        cotangent, w_down, up_act, up_val, conv_act, conv_val, bias_act, bias_val, w_act, w_val
    )
    grad_w_act, act_norms = weight_gradient(hidden_in, all_up_act)
    grad_w_val, val_norms = weight_gradient(hidden_in, all_up_val)
    grad_w_down, down_norms = weight_gradient(all_mixed, cot_columns)
    taps_act, sums_act = sums[:tap_count], sums[tap_count]
    taps_val, sums_val = sums[tap_count + 1 : 2 * tap_count + 1], sums[2 * tap_count + 1]
    tap_squares = jnp.stack(
        [jnp.sum(taps_act * taps_act, axis=1), jnp.sum(taps_val * taps_val, axis=1)], 0
    )
    depth = hidden_in.shape[1]
    flat = tap_squares.reshape(1, -1)
    stat = jnp.concatenate(
        [
            act_norms,
            val_norms,
            jnp.pad(flat, ((0, 0), (0, depth - flat.shape[1]))),
            jnp.zeros((5, depth), F32),
        ],
        0,
    )
    down_stat = jnp.pad(down_norms, ((0, 7), (0, 0)))
    grad_input, stat, down_stat = reduced(terms, stat, down_stat)
    return (
        grad_input,
        grad_w_act,
        grad_w_val,
        grad_w_down,
        taps_act,
        taps_val,
        sums_act,
        sums_val,
        stat[0],
        stat[1],
        down_stat[0],
        stat[2, : 2 * tap_count].reshape(2, tap_count),
    )


def passed_along(value, axis, by):
    length = lax.axis_size(axis)
    pairs = [(i, i + by) for i in range(length) if 0 <= i + by < length]
    return lax.ppermute(value, axis, pairs)


def contract_last(left, right):
    return lax.dot_general(
        left, right, (((1,), (1,)), ((), ())), preferred_element_type=jnp.float32
    )


def contract_first(left, right):
    return lax.dot_general(
        left, right, (((0,), (0,)), ((), ())), preferred_element_type=jnp.float32
    )


def conv_ahead(extended, taps, bias, length):
    total = jnp.zeros((length, extended.shape[1]), jnp.float32) + bias.astype(jnp.float32)
    for offset in range(taps.shape[0]):
        total = total + taps[offset].astype(jnp.float32) * extended[offset : offset + length]
    return total


def conv_behind(extended, taps, length):
    reach = taps.shape[0] - 1
    total = jnp.zeros((length, extended.shape[1]), jnp.float32)
    for offset in range(taps.shape[0]):
        total = (
            total
            + taps[offset].astype(jnp.float32) * extended[reach - offset : reach - offset + length]
        )
    return total.astype(jnp.bfloat16)


def tap_grads(grad_pre, extended, tap_count):
    length = grad_pre.shape[0]
    rows = [
        jnp.sum(grad_pre * extended[offset : offset + length], axis=0)
        for offset in range(tap_count)
    ]
    return (jnp.stack(rows, 0), jnp.sum(grad_pre, axis=0))


def per_device(
    hidden_in,
    up_act,
    up_val,
    cotangent,
    w_act,
    w_val,
    w_down,
    conv_act,
    conv_val,
    bias_act,
    bias_val,
):
    if kernels_fit(up_act, w_down, conv_act):
        return with_kernels(
            hidden_in, up_act, up_val, cotangent, w_act, w_val, w_down,
            conv_act, conv_val, bias_act, bias_val,
        )
    local_rows = cotangent.shape[0]
    tap_count = conv_act.shape[0]
    reach = tap_count - 1
    tp_count = lax.axis_size("tp")
    fs_count = lax.axis_size("fs")
    down_whole = lax.all_gather(w_down, "tp", axis=1, tiled=True)
    prev_act, prev_val = passed_along(
        (up_act[local_rows - reach :], up_val[local_rows - reach :]), "tp", 1
    )
    ext_act = jnp.concatenate([prev_act, up_act], 0).astype(jnp.float32)
    ext_val = jnp.concatenate([prev_val, up_val], 0).astype(jnp.float32)
    pre_act = conv_ahead(ext_act, conv_act, bias_act, local_rows)
    pre_val = conv_ahead(ext_val, conv_val, bias_val, local_rows)
    gelu_act, gelu_back = jax.vjp(jax.nn.gelu, pre_act)
    mixed = (gelu_act * pre_val).astype(jnp.bfloat16)
    grad_mixed = contract_last(cotangent, down_whole).astype(jnp.bfloat16)
    grad_mixed = lax.optimization_barrier(grad_mixed).astype(jnp.float32)
    grad_pre_act = gelu_back(grad_mixed * pre_val)[0]
    grad_pre_val = grad_mixed * gelu_act
    next_act, next_val = passed_along((grad_pre_act[:reach], grad_pre_val[:reach]), "tp", -1)
    grad_up_act = conv_behind(jnp.concatenate([grad_pre_act, next_act], 0), conv_act, local_rows)
    grad_up_val = conv_behind(jnp.concatenate([grad_pre_val, next_val], 0), conv_val, local_rows)
    taps_act, sums_act = tap_grads(grad_pre_act, ext_act, tap_count)
    taps_val, sums_val = tap_grads(grad_pre_val, ext_val, tap_count)
    all_up_act, all_up_val, all_mixed = (
        lax.all_gather(grad_up_act, "tp", axis=0, tiled=True),
        lax.all_gather(grad_up_val, "tp", axis=0, tiled=True),
        lax.all_gather(mixed, "tp", axis=0, tiled=True),
    )
    cot_columns = lax.all_to_all(cotangent, "tp", split_axis=1, concat_axis=0, tiled=True)
    grad_w_act = contract_first(hidden_in, all_up_act)
    grad_w_val = contract_first(hidden_in, all_up_val)
    grad_w_down = contract_first(all_mixed, cot_columns)
    shard_rows = local_rows // fs_count
    block_rows = tp_count * shard_rows

    def select_rows(gathered):
        shaped = gathered.reshape(tp_count, fs_count, shard_rows, gathered.shape[1])
        return jnp.transpose(shaped, (1, 0, 2, 3)).reshape(
            lax.axis_size("fs") * block_rows, gathered.shape[1]
        )

    summed = lax.psum_scatter(
        contract_last(select_rows(all_up_act), w_act)
        + contract_last(select_rows(all_up_val), w_val),
        "fs",
        scatter_dimension=0,
        tiled=True,
    ).astype(jnp.bfloat16)
    grad_input = lax.all_to_all(summed, "tp", split_axis=0, concat_axis=1, tiled=True)
    down_squares = jnp.sum(grad_w_down * grad_w_down, axis=1)
    taps_act, taps_val, sums_act, sums_val, rows_down = lax.psum(
        (taps_act, taps_val, sums_act, sums_val, down_squares), "tp"
    )
    tap_squares = jnp.stack(
        [jnp.sum(taps_act * taps_act, axis=1), jnp.sum(taps_val * taps_val, axis=1)], 0
    )
    rows_act, rows_val, conv_rows = lax.psum(
        (
            jnp.sum(grad_w_act * grad_w_act, axis=1),
            jnp.sum(grad_w_val * grad_w_val, axis=1),
            tap_squares,
        ),
        "fs",
    )
    return (
        grad_input,
        grad_w_act,
        grad_w_val,
        grad_w_down,
        taps_act,
        taps_val,
        sums_act,
        sums_val,
        rows_act,
        rows_val,
        rows_down,
        conv_rows,
    )


def solution(mesh):
    return jax.shard_map(
        per_device,
        mesh=mesh,
        in_specs=(
            P(None, "tp"),
            P("tp", "fs"),
            P("tp", "fs"),
            P("tp", None),
            P("tp", "fs"),
            P("tp", "fs"),
            P("fs", "tp"),
            P(None, "fs"),
            P(None, "fs"),
            P("fs"),
            P("fs"),
        ),
        out_specs=(
            P(("tp", "fs"), None),
            P("tp", "fs"),
            P("tp", "fs"),
            P("fs", "tp"),
            P(None, "fs"),
            P(None, "fs"),
            P("fs"),
            P("fs"),
            P("tp"),
            P("tp"),
            P("fs"),
            P(),
        ),
        check_vma=False,
    )
```
